256 devices in a mesh: fs: 64 (over z, x, core), tp: 4 (over y).
Axes of the slice: x: 4, y: 4, z: 8, core: 2. Of those that a mesh axis runs over, the one named last changes fastest.
Arguments:
- tokens: bfloat16 [768, 4, 2048], P(None, 'tp'), may hold values from -6 to 6
- norm_gain: float32 [2048], P('fs'), may hold values from 0.1 to 1.9
- gate_weight: float32 [8, 2048, 4096], P(None, 'fs', 'tp'), may hold values from -0.125 to 0.125
- up_weight: float32 [8, 2048, 4096], P(None, 'fs', 'tp'), may hold values from -0.125 to 0.125
- down_weight: float32 [8, 2048, 4096], P(None, 'fs', 'tp'), may hold values from -0.09375 to 0.09375
- expert_ids: int32 [768, 4, 2], P(None, 'tp'), may hold values from 0 to 7, all different within a row
- expert_mix: float32 [768, 4, 2], P(None, 'tp'), may hold values from 0.2 to 1
Outputs:
- gate_serve: bfloat16 [8, 2048, 4096], P(None, None, 'fs')
- up_serve: bfloat16 [8, 2048, 4096], P(None, None, 'fs')
- down_serve: bfloat16 [8, 2048, 4096], P(None, None, 'fs')
- mixed: bfloat16 [768, 4, 2048], P('fs', 'tp')
The draws below stay inside these ranges and needn't reach their ends.
Inputs may be any that keep to these rules, and one draw needn't show every extreme that they name: `expert_ids`: each token names two different experts.
All inputs are finite; a program needn't handle non-finite values.
Results may differ from the reference program's by a relative error of at most 0.0082.
Values may be sent and summed in bfloat16 or wider, within the bound.
A program may use at most 64 MiB of HBM per device.

```python
import jax
import jax.numpy as jnp
from jax import lax

D = 2048
FF = 4096
EXPERTS = 8
ROWS = 768
N_TP = 4


def shard_levels(rng, shape, pieces, smallest, top_value):
    gain, own = 1.0, jax.random.fold_in(rng, 6)
    for axis_at, parts in pieces:
        heights = jnp.exp(jax.random.uniform(jax.random.fold_in(own, axis_at), (parts,), jnp.float32, smallest / len(pieces), top_value / len(pieces)))
        gain = gain * jnp.repeat(heights, shape[axis_at] // parts).reshape([-1 if axis == axis_at else 1 for axis in range(len(shape))])
    return gain


def picks_of(key, rows, count, top, lift):
    order = jax.random.permutation(jax.random.fold_in(key, 1), count)
    pull = order
    for power in range(3):
        pull = pull * pull // count
    pull = pull * lift // count
    tickets = jax.random.randint(jax.random.fold_in(key, 2), (rows, count), 0, 4096) + pull
    fixed_rows = jax.random.permutation(jax.random.fold_in(key, 3), rows)[jnp.arange(count) % rows]
    tickets = jnp.where(jnp.arange(rows)[:, None] == fixed_rows[None, :], 1 << 14, tickets)
    priority = tickets * count + jnp.arange(count)
    return lax.top_k(priority.astype(jnp.int32), top)[1].astype(jnp.int32)


def normal_values(rng, dims, deviation, reach, pieces=(), held_as=jnp.bfloat16):
    entries = jax.random.normal(rng, dims, jnp.float32) * deviation
    if len(pieces) > 0:
        entries = shard_levels(rng, dims, pieces, -0.22, 0.18) * entries
    return jnp.clip(entries, min=-reach, max=reach).astype(held_as)


def setup_inputs(seed: int = 0) -> dict:
    key_of = jax.random.split(jax.random.key(seed), 8)
    tokens = normal_values(key_of[0], (ROWS, N_TP, D), 1.0, 6.0, ((1, 4),))
    norm_gain = jnp.clip(1.0 + 0.18 * jax.random.normal(key_of[1], (D,), jnp.float32), 0.1, 1.9)
    gate_weight = normal_values(key_of[2], (EXPERTS, D, FF), D ** -0.5, 0.125, ((1, 64), (2, 4)), jnp.float32)
    up_weight = normal_values(key_of[3], (EXPERTS, D, FF), D ** -0.5, 0.125, ((1, 64), (2, 4)), jnp.float32)
    down_weight = normal_values(key_of[4], (EXPERTS, D, FF), FF ** -0.5, 0.09375, ((1, 64), (2, 4)), jnp.float32)
    expert_ids = picks_of(key_of[5], ROWS * N_TP, EXPERTS, 2, 0).reshape((ROWS, N_TP, 2))
    expert_mix = jnp.clip(0.2 + 0.8 * jax.random.uniform(key_of[6], (ROWS, N_TP, 2), jnp.float32) ** shard_levels(key_of[6], (ROWS, N_TP, 2), ((1, 4),), -0.2, 0.2), 0.2, 1.0)
    return dict(tokens=tokens, norm_gain=norm_gain, gate_weight=gate_weight, up_weight=up_weight, down_weight=down_weight, expert_ids=expert_ids, expert_mix=expert_mix)


norm_eps = 1e-05

def reference(tokens, norm_gain, gate_weight, up_weight, down_weight, expert_ids, expert_mix):
    gate_serve = (gate_weight * norm_gain[None, :, None]).astype(jnp.bfloat16)
    up_serve = (up_weight * norm_gain[None, :, None]).astype(jnp.bfloat16)
    down_serve = down_weight.astype(jnp.bfloat16)
    token_rows = tokens.reshape(-1, D).astype(jnp.float32)
    row_mean = lax.optimization_barrier(jnp.mean(token_rows, axis=1, keepdims=True))
    centered = token_rows - row_mean
    variance = lax.optimization_barrier(jnp.mean(centered * centered, axis=1, keepdims=True))
    normed = (centered * lax.rsqrt(variance + norm_eps)).astype(jnp.bfloat16)
    route_ids = expert_ids.reshape(-1, 2)
    route_mix = expert_mix.reshape(-1, 2)
    expert_iota = jnp.arange(EXPERTS, dtype=jnp.int32)
    expert_gates = lax.optimization_barrier(jnp.sum((route_ids[:, :, None] == expert_iota[None, None, :]).astype(jnp.float32) * route_mix[:, :, None], axis=1))

    def add_expert(running, weights_now):
        gate_mat, up_mat, down_mat, gate_col = weights_now
        gate_act = jnp.dot(normed, gate_mat, preferred_element_type=jnp.float32)
        up_act = jnp.dot(normed, up_mat, preferred_element_type=jnp.float32)
        hidden = (jax.nn.silu(gate_act) * up_act * gate_col[:, None]).astype(jnp.bfloat16)
        product = lax.dot_general(hidden, down_mat, (((1,), (1,)), ((), ())), preferred_element_type=jnp.float32)
        return (running + product, None)
    start_sum = jnp.zeros((token_rows.shape[0], D), jnp.float32)
    summed, _ = lax.scan(add_expert, start_sum, (gate_serve, up_serve, down_serve, expert_gates.T))
    mixed = summed.astype(jnp.bfloat16).reshape(ROWS, N_TP, D)
    return (gate_serve, up_serve, down_serve, mixed)
```

```python
import functools

import jax
import jax.numpy as jnp
from jax import lax
from jax.experimental import pallas as pl
from jax.experimental.pallas import tpu as pltpu
from jax.sharding import Mesh
from jax.sharding import PartitionSpec as P

FS = ("fs_0", "fs_1", "fs_2")
NZ, NX, NC, NY = 8, 4, 2, 4
NXC = NX * NC
MESH = pl.DeviceIdType.MESH


norm_eps = 1e-05


def remote(src, dst, send, recv, **where):
    return pltpu.make_async_remote_copy(
        src_ref=src, dst_ref=dst, send_sem=send, recv_sem=recv, device_id=where, device_id_type=MESH
    )


def greet(peers):
    barrier = pltpu.get_barrier_semaphore()
    for where in peers:
        pl.semaphore_signal(barrier, inc=1, device_id=where, device_id_type=MESH)
    pl.semaphore_wait(barrier, len(peers))


def weights_kernel(
    gain_ref, gate_hbm, up_hbm, down_hbm, gate_out, up_out, down_out,
    win, packed, by_plane, by_z, rows, turned,
    in_sem, out_sem, y_send, y_recv, z_send, z_recv, x_send, x_recv, g_send, g_recv,
):
    z, x, c, y = (lax.axis_index(a) for a in ("fs_0", "fs_1", "fs_2", "tp"))
    xc = x * NC + c
    loads = [
        pltpu.make_async_copy(ref, win.at[w], in_sem.at[w])
        for w, ref in enumerate((gate_hbm, up_hbm, down_hbm))
    ]
    for load in loads:
        load.start()

    def z_of(j):
        return lax.rem(z + j, NZ)

    def y_of(j):
        return lax.rem(y + j, NY)

    def xc_of(j):
        to = lax.rem(xc + j, NXC)
        return to, {"fs_1": lax.div(to, NC), "fs_2": lax.rem(to, NC)}

    greet(
        [{"tp": y_of(j)} for j in range(1, NY)]
        + [{"fs_0": z_of(j)} for j in range(1, NZ)]
        + [xc_of(j)[1] for j in range(1, NXC)]
    )

    sent = []

    def go(copy):
        copy.start()
        sent.append(copy)
        return copy

    left_lanes = lax.broadcasted_iota(jnp.int32, (32, 128), 1) < 64

    def fold(w):
        loads[w].wait()

        def block(j, carry):
            at = pl.ds(pl.multiple_of(j * 128, 128), 128)
            for g in range(NY):
                one = win[w, 2 * g, :, at]
                two = win[w, 2 * g + 1, :, at]
                if w < 2:
                    one, two = one * gain_ref[...], two * gain_ref[...]
                first = jnp.where(left_lanes, one, pltpu.roll(two, 64, 1))
                second = jnp.where(left_lanes, pltpu.roll(one, 64, 1), two)
                packed[w, g, 2 * j] = first.astype(jnp.bfloat16)
                packed[w, g, 2 * j + 1] = second.astype(jnp.bfloat16)
            return carry

        lax.fori_loop(0, 8, block, 0)

    def y_copies(w):
        return [
            remote(
                packed.at[w, y_of(j)], by_plane.at[w, y],
                y_send.at[w, j - 1], y_recv.at[w, j - 1], tp=y_of(j),
            )
            for j in (1, 3, 2)
        ]

    def z_copies(w):
        copies = []
        for j in (1, 7, 2, 6, 3, 5, 4):
            to = z_of(j)
            half = lax.rem(to, 2) * 8
            copies.append(
                remote(
                    by_plane.at[w, lax.div(to, 2), pl.ds(half, 8)], by_z.at[w, z],
                    z_send.at[w, j - 1], z_recv.at[w, j - 1], fs_0=to,
                )
            )
        return copies

    def x_copies(w):
        copies = []
        for j in range(1, NXC):
            to, where = xc_of(j)
            copies.append(
                remote(
                    by_z.at[w, :, to], rows.at[w, y, :, xc],
                    x_send.at[w, j - 1], x_recv.at[w, j - 1], **where,
                )
            )
        return copies

    def g_copies(w):
        return [
            remote(rows.at[w, y], rows.at[w, y], g_send.at[w, 0], g_recv.at[w, 0], tp=y_of(1)),
            remote(rows.at[w, y], rows.at[w, y], g_send.at[w, 1], g_recv.at[w, 1], tp=y_of(3)),
        ]

    def f_copies(w):
        lo = rows.at[w, y_of(3), pl.ds(0, 4)]
        hi = rows.at[w, y_of(1), pl.ds(4, 4)]
        return [
            remote(lo, lo, g_send.at[w, 2], g_recv.at[w, 2], tp=y_of(1)),
            remote(hi, hi, g_send.at[w, 3], g_recv.at[w, 3], tp=y_of(3)),
        ]

    ys, zs, xs, gs, fs = ([None] * 3 for _ in range(5))

    def wait(copies):
        for copy in copies:
            copy.wait_recv()

    def start_y(w):
        fold(w)
        ys[w] = [go(copy) for copy in y_copies(w)]
        by_plane[w, y] = packed[w, y]

    def start_z(w):
        wait(ys[w])
        zs[w] = [go(copy) for copy in z_copies(w)]
        by_z[w, z] = by_plane[w, lax.div(z, 2), pl.ds(lax.rem(z, 2) * 8, 8)]

    def start_x(w):
        wait(zs[w])
        xs[w] = [go(copy) for copy in x_copies(w)]
        rows[w, y, :, xc] = by_z[w, :, xc]

    def start_g(w):
        wait(xs[w])
        gs[w] = [go(copy) for copy in g_copies(w)]

    def start_f(w):
        wait(gs[w])
        fs[w] = [go(copy) for copy in f_copies(w)]

    def turn(w, g):
        def block(i, carry):
            tile = rows[w, g, lax.div(i, 2), pl.ds(lax.rem(i, 2) * 4, 4)]
            tile = tile.reshape(128, 128).astype(jnp.float32).T.astype(jnp.bfloat16)
            at = pl.ds(pl.multiple_of(i * 128, 128), 128)
            turned[w, g, :, at] = tile
            return carry

        lax.fori_loop(0, 16, block, 0)

    outs = (gate_out, up_out, down_out)
    stores = []

    def finish(w):
        wait(fs[w])
        turn(w, y_of(2))
        store = pltpu.make_async_copy(turned.at[w], outs[w], out_sem.at[w])
        store.start()
        stores.append(store)

    start_y(0)
    start_y(1)
    start_y(2)
    start_z(0)
    start_z(1)
    start_z(2)
    start_x(0)
    start_g(0)
    start_x(1)
    turn(0, y)
    start_g(1)
    start_f(0)
    start_x(2)
    turn(1, y)
    turn(0, y_of(1))
    turn(0, y_of(3))
    start_g(2)
    start_f(1)
    finish(0)
    turn(1, y_of(1))
    turn(1, y_of(3))
    turn(2, y)
    start_f(2)
    finish(1)
    turn(2, y_of(1))
    turn(2, y_of(3))
    finish(2)
    for copy in sent:
        copy.wait_send()
    for store in stores:
        store.wait()


def handed_over(norm_gain, gate_weight, up_weight, down_weight):
    bf16, dma = jnp.bfloat16, pltpu.SemaphoreType.DMA
    out = jax.ShapeDtypeStruct((NY, 128, 2048), bf16)
    anywhere = pl.BlockSpec(memory_space=pl.ANY)
    gain = jnp.broadcast_to(norm_gain[:, None], (32, 128))
    return pl.pallas_call(
        weights_kernel,
        out_shape=(out, out, out),
        in_specs=[pl.BlockSpec(memory_space=pltpu.VMEM), anywhere, anywhere, anywhere],
        out_specs=(anywhere, anywhere, anywhere),
        scratch_shapes=[
            pltpu.VMEM((3, 8, 32, 1024), jnp.float32),
            pltpu.VMEM((3, NY, 16, 32, 128), bf16),
            pltpu.VMEM((3, NY, 16, 32, 128), bf16),
            pltpu.VMEM((3, NZ, NXC, 32, 128), bf16),
            pltpu.VMEM((3, NY, NZ, NXC, 32, 128), bf16),
            pltpu.VMEM((3, NY, 128, 2048), bf16),
            dma((3,)), dma((3,)),
            dma((3, 3)), dma((3, 3)),
            dma((3, 7)), dma((3, 7)),
            dma((3, 7)), dma((3, 7)),
            dma((3, 4)), dma((3, 4)),
        ],
        compiler_params=pltpu.CompilerParams(
            collective_id=0, has_side_effects=True, vmem_limit_bytes=56 * 2**20
        ),
        name="weights",
    )(gain, gate_weight, up_weight, down_weight)


def sum_kernel(
    part, out_ref, pair_in, chip, xa_in, xb_in, mine, z_in, piece, other,
    p_send, p_recv, x_send, x_recv, z_send, z_recv, o_send, o_recv,
):
    z, x, c = (lax.axis_index(a) for a in FS)
    f32, bf16 = jnp.float32, jnp.bfloat16
    right, left, far = (lax.rem(x + j, NX) for j in (1, 3, 2))

    def z_of(j):
        return lax.rem(z + j, NZ)

    greet(
        [{"fs_2": 1 - c}, {"fs_1": right}, {"fs_1": left}]
        + [{"fs_0": z_of(j)} for j in range(1, NZ)]
    )
    sent = []

    def go(copy):
        copy.start()
        sent.append(copy)
        return copy

    def columns(of):
        return pl.ds(pl.multiple_of(of * 1024, 1024), 1024)

    pair = go(remote(part.at[:, :, :, columns(1 - c)], pair_in, p_send, p_recv, fs_2=1 - c))
    pair.wait_recv()

    def add_pair(i, carry):
        for j in range(NX):
            own = part[i, j, :, columns(c)].astype(f32)
            chip[i, j] = (own + pair_in[i, j].astype(f32)).astype(bf16)
        return carry

    lax.fori_loop(0, NZ, add_pair, 0)
    lo, hi = pl.ds(0, 4), pl.ds(4, 4)
    far_r = go(remote(chip.at[lo, far], xa_in.at[0], x_send.at[0], x_recv.at[0], fs_1=right))
    far_l = go(remote(chip.at[hi, far], xb_in.at[0], x_send.at[1], x_recv.at[1], fs_1=left))
    own_r = go(remote(chip.at[hi, right], xa_in.at[2], x_send.at[2], x_recv.at[2], fs_1=right))
    own_l = go(remote(chip.at[lo, left], xb_in.at[2], x_send.at[3], x_recv.at[3], fs_1=left))

    def add_far(start, to, got):
        def step(i, carry):
            chip[start + i, to] = (
                chip[start + i, to].astype(f32) + got[0, i].astype(f32)
            ).astype(bf16)
            return carry

        lax.fori_loop(0, 4, step, 0)

    far_r.wait_recv()
    add_far(0, right, xa_in)
    sum_r = go(remote(chip.at[lo, right], xa_in.at[1], x_send.at[4], x_recv.at[4], fs_1=right))
    far_l.wait_recv()
    add_far(4, left, xb_in)
    sum_l = go(remote(chip.at[hi, left], xb_in.at[1], x_send.at[5], x_recv.at[5], fs_1=left))
    own_r.wait_recv()
    own_l.wait_recv()
    sum_r.wait_recv()
    sum_l.wait_recv()

    def add_x(i, carry):
        mine[i] = (
            chip[i, x].astype(f32) + xa_in[1, i].astype(f32) + xb_in[2, i].astype(f32)
        ).astype(bf16)
        mine[4 + i] = (
            chip[4 + i, x].astype(f32) + xa_in[2, i].astype(f32) + xb_in[1, i].astype(f32)
        ).astype(bf16)
        return carry

    lax.fori_loop(0, 4, add_x, 0)
    zs = [
        go(remote(mine.at[z_of(j)], z_in.at[j - 1], z_send.at[j - 1], z_recv.at[j - 1], fs_0=z_of(j)))
        for j in (1, 7, 2, 6, 3, 5, 4)
    ]
    for copy in zs:
        copy.wait_recv()
    total = mine[z].astype(f32)
    for j in range(7):
        total = total + z_in[j].astype(f32)
    piece[...] = total.astype(bf16)
    last = go(remote(piece, other, o_send, o_recv, fs_2=1 - c))
    last.wait_recv()
    here, there = piece[...].astype(f32), other[...].astype(f32)
    here = jnp.where(c == 0, here[:12], here[12:])
    there = jnp.where(c == 0, there[:12], there[12:])
    out_ref[:, :1024] = jnp.where(c == 0, here, there).astype(bf16)
    out_ref[:, 1024:] = jnp.where(c == 0, there, here).astype(bf16)
    for copy in sent:
        copy.wait_send()


def summed_rows(part):
    bf16, dma = jnp.bfloat16, pltpu.SemaphoreType.DMA
    return pl.pallas_call(
        sum_kernel,
        out_shape=jax.ShapeDtypeStruct((12, 2048), bf16),
        in_specs=[pl.BlockSpec(memory_space=pltpu.VMEM)],
        out_specs=pl.BlockSpec(memory_space=pltpu.VMEM),
        scratch_shapes=[
            pltpu.VMEM((NZ, NX, 24, 1024), bf16),
            pltpu.VMEM((NZ, NX, 24, 1024), bf16),
            pltpu.VMEM((3, 4, 24, 1024), bf16),
            pltpu.VMEM((3, 4, 24, 1024), bf16),
            pltpu.VMEM((NZ, 24, 1024), bf16),
            pltpu.VMEM((7, 24, 1024), bf16),
            pltpu.VMEM((24, 1024), bf16),
            pltpu.VMEM((24, 1024), bf16),
            dma, dma, dma((6,)), dma((6,)), dma((7,)), dma((7,)), dma, dma,
        ],
        compiler_params=pltpu.CompilerParams(
            collective_id=1, has_side_effects=True, vmem_limit_bytes=40 * 2**20
        ),
        name="sums",
    )(part.reshape(NZ, NX, 24, 2048))


def local(tokens, norm_gain, gate_weight, up_weight, down_weight, expert_ids, expert_mix):
    gate_serve, up_serve, down_serve = (
        jnp.swapaxes(a.reshape(8, 64, 2048), 1, 2)
        for a in handed_over(norm_gain, gate_weight, up_weight, down_weight)
    )
    width = tokens.shape[2]
    token_rows = tokens.reshape(-1, width).astype(jnp.float32)
    row_mean = jnp.mean(token_rows, axis=1, keepdims=True)
    centered = token_rows - row_mean
    variance = jnp.mean(centered * centered, axis=1, keepdims=True)
    normed = (centered * lax.rsqrt(variance + norm_eps)).astype(jnp.bfloat16)
    route_ids = expert_ids.reshape(-1, 2)
    route_mix = expert_mix.reshape(-1, 2)
    expert_iota = jnp.arange(gate_serve.shape[0], dtype=jnp.int32)
    expert_gates = jnp.sum(
        (route_ids[:, :, None] == expert_iota[None, None, :]).astype(jnp.float32)
        * route_mix[:, :, None],
        axis=1,
    )
    gate_act = jnp.einsum("rd,edf->ref", normed, gate_serve, preferred_element_type=jnp.float32)
    up_act = jnp.einsum("rd,edf->ref", normed, up_serve, preferred_element_type=jnp.float32)
    hidden = (jax.nn.silu(gate_act) * up_act * expert_gates[:, :, None]).astype(jnp.bfloat16)
    part = jnp.einsum("ref,edf->rd", hidden, down_serve, preferred_element_type=jnp.float32)
    mixed = summed_rows(part.astype(jnp.bfloat16)).reshape(12, 1, width)
    return (gate_serve, up_serve, down_serve, mixed)


def solution(mesh):
    finer = Mesh(mesh.devices.reshape(NZ, NX, NC, mesh.shape["tp"]), ("fs_0", "fs_1", "fs_2", "tp"))
    placed = (
        P(None, "tp", None),
        P(FS),
        P(None, FS, "tp"),
        P(None, FS, "tp"),
        P(None, FS, "tp"),
        P(None, "tp", None),
        P(None, "tp", None),
    )
    return jax.shard_map(
        local,
        mesh=finer,
        in_specs=placed,
        out_specs=(P(None, None, FS), P(None, None, FS), P(None, None, FS), P(FS, "tp", None)),
        check_vma=False,
    )
```

```python
import functools

import jax
import jax.numpy as jnp
from jax import lax
from jax.experimental import pallas as pl
from jax.experimental.pallas import tpu as pltpu
from jax.sharding import Mesh
from jax.sharding import PartitionSpec as P

FS = ("fs_0", "fs_1", "fs_2")
NZ, NX, NC, NY = 8, 4, 2, 4
NXC = NX * NC
MESH = pl.DeviceIdType.MESH


NH, NQ = 2, 4
HR = 32 // NH
QC = 2048 // NQ

norm_eps = 1e-05


def remote(src, dst, send, recv, **where):
    return pltpu.make_async_remote_copy(
        src_ref=src, dst_ref=dst, send_sem=send, recv_sem=recv, device_id=where, device_id_type=MESH
    )


def layer_kernel(
    tok_hbm, gain_ref, gate_hbm, up_hbm, down_hbm, ids_ref, mix_ref,
    gate_out, up_out, down_out, mixed_ref,
    win, packed, by_plane, by_z, rows, turned, normed, square, route, hidden,
    part, pair_in, chip, x_in, mine, z_in, piece, other,
    in_sem, out_sem, y_send, y_recv, z_send, z_recv, x_send, x_recv, g_send, g_recv,
    d_send, d_recv, p_send, p_recv, s_send, s_recv, t_send, t_recv, o_send, o_recv,
):
    z, x, c, y = (lax.axis_index(a) for a in ("fs_0", "fs_1", "fs_2", "tp"))
    xc = x * NC + c
    f32, bf16 = jnp.float32, jnp.bfloat16
    loads = [
        pltpu.make_async_copy(ref, win.at[w], in_sem.at[w])
        for w, ref in enumerate((gate_hbm, up_hbm, down_hbm))
    ]
    loads.append(pltpu.make_async_copy(tok_hbm, normed, in_sem.at[3]))
    for load in loads:
        load.start()

    def z_of(j):
        return lax.rem(z + j, NZ)

    def y_of(j):
        return lax.rem(y + j, NY)

    def x_of(j):
        return lax.rem(x + j, NX)

    def xc_of(j):
        to = lax.rem(xc + j, NXC)
        return to, {"fs_1": lax.div(to, NC), "fs_2": lax.rem(to, NC)}

    sent = []

    def go(copies):
        for copy in copies:
            copy.start()
            sent.append(copy)
        return copies

    def wait(copies):
        for copy in copies:
            copy.wait_recv()

    left_lanes = lax.broadcasted_iota(jnp.int32, (32, 128), 1) < 64
    left_half = lax.broadcasted_iota(jnp.int32, (1, 128), 1) < 64

    square[...] = jnp.zeros_like(square)
    square[:, :32] = jnp.broadcast_to(gain_ref[...], (128, 32))
    gain = square[...].T[:32]
    square[:32] = gain

    def fold(w):
        loads[w].wait()

        def block(j, carry):
            at = pl.ds(pl.multiple_of(j * 128, 128), 128)
            for g in range(NY):
                one = win[w, 2 * g, :, at]
                two = win[w, 2 * g + 1, :, at]
                if w < 2:
                    one, two = one * square[:32], two * square[:32]
                first = jnp.where(left_lanes, one, pltpu.roll(two, 64, 1))
                second = jnp.where(left_lanes, pltpu.roll(one, 64, 1), two)
                packed[w, g, 2 * j] = first.astype(bf16)
                packed[w, g, 2 * j + 1] = second.astype(bf16)
            return carry

        lax.fori_loop(0, 8, block, 0)

    def part_of(h):
        return pl.ds(h * HR, HR)

    def y_copies(w, h):
        return [
            remote(
                packed.at[w, y_of(j), :, part_of(h)], by_plane.at[w, y, :, part_of(h)],
                y_send.at[w, h, j - 1], y_recv.at[w, h, j - 1], tp=y_of(j),
            )
            for j in (1, 3, 2)
        ]

    def z_copies(w, h):
        copies = []
        for j in (1, 7, 2, 6, 3, 5, 4):
            to = z_of(j)
            half = lax.rem(to, 2) * 8
            copies.append(
                remote(
                    by_plane.at[w, lax.div(to, 2), pl.ds(half, 8), part_of(h)],
                    by_z.at[w, z, :, part_of(h)],
                    z_send.at[w, h, j - 1], z_recv.at[w, h, j - 1], fs_0=to,
                )
            )
        return copies

    def x_copies(w, h):
        copies = []
        for j in range(1, NXC):
            to, where = xc_of(j)
            copies.append(
                remote(
                    by_z.at[w, :, to, part_of(h)], rows.at[w, y, :, xc, part_of(h)],
                    x_send.at[w, h, j - 1], x_recv.at[w, h, j - 1], **where,
                )
            )
        return copies

    def g_copies(w, h):
        own = rows.at[w, y, :, :, part_of(h)]
        return [
            remote(own, own, g_send.at[w, h, 0], g_recv.at[w, h, 0], tp=y_of(1)),
            remote(own, own, g_send.at[w, h, 1], g_recv.at[w, h, 1], tp=y_of(3)),
        ]

    def f_copies(w, h):
        lo = rows.at[w, y_of(3), pl.ds(0, 4), :, part_of(h)]
        hi = rows.at[w, y_of(1), pl.ds(4, 4), :, part_of(h)]
        return [
            remote(lo, lo, g_send.at[w, h, 2], g_recv.at[w, h, 2], tp=y_of(1)),
            remote(hi, hi, g_send.at[w, h, 3], g_recv.at[w, h, 3], tp=y_of(3)),
        ]

    QZ = NZ // NQ

    def dg_copies(q):
        own = rows.at[2, y, pl.ds(q * QZ, QZ)]
        return [
            remote(own, own, d_send.at[q, 0], d_recv.at[q, 0], tp=y_of(1)),
            remote(own, own, d_send.at[q, 1], d_recv.at[q, 1], tp=y_of(3)),
        ]

    def df_copies(q):
        lo = rows.at[2, y_of(3), pl.ds(q * QZ, QZ // 2)]
        hi = rows.at[2, y_of(1), pl.ds(q * QZ + QZ // 2, QZ // 2)]
        return [
            remote(lo, lo, d_send.at[q, 2], d_recv.at[q, 2], tp=y_of(1)),
            remote(hi, hi, d_send.at[q, 3], d_recv.at[q, 3], tp=y_of(3)),
        ]

    ys, zs, xs, gs, fs = ({} for _ in range(5))
    dg, df, pairs, sums, tops, ends = ({} for _ in range(6))

    def start_y(w, h):
        ys[w, h] = go(y_copies(w, h))
        by_plane[w, y, :, part_of(h)] = packed[w, y, :, part_of(h)]

    def start_z(w, h):
        wait(ys[w, h])
        zs[w, h] = go(z_copies(w, h))
        half = pl.ds(lax.rem(z, 2) * 8, 8)
        by_z[w, z, :, part_of(h)] = by_plane[w, lax.div(z, 2), half, part_of(h)]

    def start_x(w, h):
        wait(zs[w, h])
        xs[w, h] = go(x_copies(w, h))
        rows[w, y, :, xc, part_of(h)] = by_z[w, :, xc, part_of(h)]

    def start_g(w, h):
        wait(xs[w, h])
        gs[w, h] = go(g_copies(w, h))

    def start_f(w, h):
        wait(gs[w, h])
        fs[w, h] = go(f_copies(w, h))

    def start_dg(q):
        dg[q] = go(dg_copies(q))

    def start_df(q):
        wait(dg[q])
        df[q] = go(df_copies(q))

    def spread(i, carry):
        at = pl.ds(pl.multiple_of(i * 128, 128), 128)
        for k in range(2):
            wide = jnp.broadcast_to(ids_ref[k : k + 1, at].astype(f32), (128, 128))
            route[k, at] = wide.T
            wide = jnp.broadcast_to(mix_ref[k : k + 1, at], (128, 128))
            route[2 + k, at] = wide.T
        return carry

    def normalize(start, stop):
        def block(i, carry):
            at = pl.ds(pl.multiple_of(i * 64, 64), 64)
            values = normed[at].astype(f32)
            centered = values - jnp.mean(values, axis=1, keepdims=True)
            variance = jnp.mean(centered * centered, axis=1, keepdims=True)
            normed[at] = (centered * lax.rsqrt(variance + norm_eps)).astype(bf16)
            return carry

        lax.fori_loop(start, stop, block, 0)

    def turn(w, g):
        def block(i, carry):
            for k in range(2):
                tile = rows[w, g, 2 * i + k].reshape(256, 128).astype(f32).T.astype(bf16)
                at = pl.ds(pl.multiple_of(i * 512 + k * 256, 256), 256)
                turned[w, g, :, at] = tile
            return carry

        lax.fori_loop(0, 4, block, 0)

    outs = (gate_out, up_out, down_out)
    stores = []

    def store(w):
        copy = pltpu.make_async_copy(turned.at[w], outs[w], out_sem.at[w])
        copy.start()
        stores.append(copy)

    def hidden_of(g):
        both = jnp.concatenate(
            [rows[0, g].reshape(2048, 128), rows[1, g].reshape(2048, 128)], axis=1
        )
        expert = jnp.where(left_half, 2 * g, 2 * g + 1).astype(f32)

        def block(i, carry):
            at = pl.ds(pl.multiple_of(i * 256, 256), 256)
            acts = jnp.dot(normed[at], both, preferred_element_type=f32)
            gate_act, up_act = acts[:, :128], acts[:, 128:]
            weight = jnp.where(route[0, at] == expert, route[2, at], 0.0)
            weight = weight + jnp.where(route[1, at] == expert, route[3, at], 0.0)
            value = gate_act / (1.0 + jnp.exp(-gate_act)) * up_act * weight
            hidden[at, pl.ds(pl.multiple_of(g * 128, 128), 128)] = value.astype(bf16)
            return carry

        lax.fori_loop(0, 3, block, 0)

    def columns(of):
        return pl.ds(pl.multiple_of(of * (QC // 2), 128), QC // 2)

    def partial_of(q):
        wait(df[q])
        down = jnp.concatenate(
            [rows[2, g, pl.ds(q * QZ, QZ)].reshape(QC, 128) for g in range(NY)], axis=1
        )

        def block(i, carry):
            at = pl.ds(pl.multiple_of(i * 384, 384), 384)
            value = lax.dot_general(
                hidden[at], down, (((1,), (1,)), ((), ())), preferred_element_type=f32
            )
            part[q, pl.ds(i * 4, 4)] = value.reshape(4, NX, 24, QC).astype(bf16)
            return carry

        lax.fori_loop(0, 2, block, 0)
        pairs[q] = go(
            [remote(part.at[q, :, :, :, columns(1 - c)], pair_in.at[q], p_send.at[q], p_recv.at[q], fs_2=1 - c)]
        )

    def start_sums(q):
        wait(pairs[q])

        def add(i, carry):
            for j in range(NX):
                own = part[q, i, j, :, columns(c)].astype(f32)
                chip[q, j, i] = (own + pair_in[q, i, j].astype(f32)).astype(bf16)
            return carry

        lax.fori_loop(0, NZ, add, 0)
        sums[q] = go(
            [
                remote(chip.at[q, x_of(j)], x_in.at[q, j - 1], s_send.at[q, j - 1], s_recv.at[q, j - 1], fs_1=x_of(j))
                for j in (1, 3, 2)
            ]
        )

    def start_tops(q):
        wait(sums[q])

        def add(i, carry):
            value = chip[q, x, i].astype(f32)
            for j in range(3):
                value = value + x_in[q, j, i].astype(f32)
            mine[q, i] = value.astype(bf16)
            return carry

        lax.fori_loop(0, NZ, add, 0)
        tops[q] = go(
            [
                remote(mine.at[q, z_of(j)], z_in.at[q, j - 1], t_send.at[q, j - 1], t_recv.at[q, j - 1], fs_0=z_of(j))
                for j in (4, 3, 5, 2, 6, 1, 7)
            ]
        )

    def start_ends(q):
        wait(tops[q])
        total = mine[q, z].astype(f32)
        for j in range(7):
            total = total + z_in[q, j].astype(f32)
        piece[q] = total.astype(bf16)
        ends[q] = go([remote(piece.at[q], other.at[q], o_send.at[q], o_recv.at[q], fs_2=1 - c)])

    def finish(q):
        wait(ends[q])
        here, there = piece[q].astype(f32), other[q].astype(f32)
        here = jnp.where(c == 0, here[:12], here[12:])
        there = jnp.where(c == 0, there[:12], there[12:])
        wide = QC // 2
        mixed_ref[:, q * QC : q * QC + wide] = jnp.where(c == 0, here, there).astype(bf16)
        mixed_ref[:, q * QC + wide : (q + 1) * QC] = jnp.where(c == 0, there, here).astype(bf16)

    barrier = pltpu.get_barrier_semaphore()
    peers = (
        [{"tp": y_of(j)} for j in range(1, NY)]
        + [{"fs_0": z_of(j)} for j in range(1, NZ)]
        + [xc_of(j)[1] for j in range(1, NXC)]
    )
    for where in peers:
        pl.semaphore_signal(barrier, inc=1, device_id=where, device_id_type=MESH)
    fold(0)
    pl.semaphore_wait(barrier, len(peers))

    start_y(0, 0)
    start_y(0, 1)
    fold(1)
    start_y(1, 0)
    start_y(1, 1)
    fold(2)
    start_y(2, 0)
    start_y(2, 1)
    start_z(0, 0)
    lax.fori_loop(0, 6, spread, 0)
    loads[3].wait()
    start_z(0, 1)
    normalize(0, 4)
    start_z(1, 0)
    normalize(4, 8)
    start_z(1, 1)
    normalize(8, 12)
    start_x(0, 0)
    start_z(2, 0)
    start_z(2, 1)
    start_g(0, 0)
    start_x(0, 1)
    start_g(0, 1)
    start_x(1, 0)
    turn(0, y)
    start_f(0, 0)
    start_g(1, 0)
    start_x(1, 1)
    start_f(0, 1)
    start_g(1, 1)
    start_x(2, 0)
    turn(1, y)
    turn(0, y_of(1))
    start_f(1, 0)
    turn(0, y_of(3))
    start_x(2, 1)
    hidden_of(y)
    wait(fs[0, 0])
    wait(fs[0, 1])
    wait(xs[2, 0])
    wait(xs[2, 1])
    start_dg(0)
    start_f(1, 1)
    start_dg(1)
    hidden_of(y_of(1))
    start_df(0)
    start_dg(2)
    hidden_of(y_of(3))
    start_df(1)
    start_dg(3)
    turn(0, y_of(2))
    store(0)
    wait(fs[1, 0])
    wait(fs[1, 1])
    hidden_of(y_of(2))
    start_df(2)
    partial_of(0)
    turn(1, y_of(1))
    start_df(3)
    partial_of(1)
    start_sums(0)
    turn(1, y_of(3))
    turn(1, y_of(2))
    store(1)
    partial_of(2)
    start_sums(1)
    start_tops(0)
    partial_of(3)
    start_sums(2)
    start_tops(1)
    start_ends(0)
    turn(2, y)
    turn(2, y_of(1))
    start_sums(3)
    start_tops(2)
    start_ends(1)
    turn(2, y_of(3))
    turn(2, y_of(2))
    store(2)
    start_tops(3)
    start_ends(2)
    finish(0)
    finish(1)
    start_ends(3)
    finish(2)
    finish(3)
    for copy in sent:
        copy.wait_send()
    for copy in stores:
        copy.wait()


def local(tokens, norm_gain, gate_weight, up_weight, down_weight, expert_ids, expert_mix):
    f32, bf16, dma = jnp.float32, jnp.bfloat16, pltpu.SemaphoreType.DMA
    out = jax.ShapeDtypeStruct((NY, 128, 2048), bf16)
    anywhere = pl.BlockSpec(memory_space=pl.ANY)
    vmem = pl.BlockSpec(memory_space=pltpu.VMEM)
    wide = QC // 2

    def both(*shape):
        return [dma(shape), dma(shape)]

    gate_serve, up_serve, down_serve, mixed = pl.pallas_call(
        layer_kernel,
        out_shape=(out, out, out, jax.ShapeDtypeStruct((12, 2048), bf16)),
        in_specs=[anywhere, vmem, anywhere, anywhere, anywhere, vmem, vmem],
        out_specs=(anywhere, anywhere, anywhere, vmem),
        scratch_shapes=[
            pltpu.VMEM((3, 8, 32, 1024), f32),
            pltpu.VMEM((3, NY, 16, 32, 128), bf16),
            pltpu.VMEM((3, NY, 16, 32, 128), bf16),
            pltpu.VMEM((3, NZ, NXC, 32, 128), bf16),
            pltpu.VMEM((3, NY, NZ, NXC, 32, 128), bf16),
            pltpu.VMEM((3, NY, 128, 2048), bf16),
            pltpu.VMEM((768, 2048), bf16),
            pltpu.VMEM((128, 128), f32),
            pltpu.VMEM((4, 768, 128), f32),
            pltpu.VMEM((768, 512), bf16),
            pltpu.VMEM((NQ, NZ, NX, 24, QC), bf16),
            pltpu.VMEM((NQ, NZ, NX, 24, wide), bf16),
            pltpu.VMEM((NQ, NX, NZ, 24, wide), bf16),
            pltpu.VMEM((NQ, 3, NZ, 24, wide), bf16),
            pltpu.VMEM((NQ, NZ, 24, wide), bf16),
            pltpu.VMEM((NQ, 7, 24, wide), bf16),
            pltpu.VMEM((NQ, 24, wide), bf16),
            pltpu.VMEM((NQ, 24, wide), bf16),
            dma((4,)), dma((3,)),
            *both(3, NH, 3), *both(3, NH, 7), *both(3, NH, 7), *both(2, NH, 4),
            *both(NQ, 4), *both(NQ), *both(NQ, 3), *both(NQ, 7), *both(NQ),
        ],
        compiler_params=pltpu.CompilerParams(
            collective_id=0, has_side_effects=True, vmem_limit_bytes=56 * 2**20
        ),
        name="layer",
    )(
        tokens.reshape(768, 2048), norm_gain.reshape(1, 32), gate_weight, up_weight, down_weight,
        expert_ids.reshape(768, 2).T, expert_mix.reshape(768, 2).T,
    )
    gate_serve, up_serve, down_serve = (
        jnp.swapaxes(a.reshape(8, 64, 2048), 1, 2) for a in (gate_serve, up_serve, down_serve)
    )
    return (gate_serve, up_serve, down_serve, mixed.reshape(12, 1, 2048))


def solution(mesh):
    finer = Mesh(mesh.devices.reshape(NZ, NX, NC, mesh.shape["tp"]), ("fs_0", "fs_1", "fs_2", "tp"))
    placed = (
        P(None, "tp", None),
        P(FS),
        P(None, FS, "tp"),
        P(None, FS, "tp"),
        P(None, FS, "tp"),
        P(None, "tp", None),
        P(None, "tp", None),
    )
    return jax.shard_map(
        local,
        mesh=finer,
        in_specs=placed,
        out_specs=(P(None, None, FS), P(None, None, FS), P(None, None, FS), P(FS, "tp", None)),
        check_vma=False,
    )
```
